32 devices in a mesh: ep: 4 (over y, x), tp: 8 (over z, core).
Axes of the slice: x: 2, y: 2, z: 4, core: 2. Of those that a mesh axis runs over, the one named last changes fastest.
Arguments:
- tokens: bfloat16 [512, 2048], P('ep'), may hold values from -6 to 6
- conv_state: bfloat16 [512, 3, 2048], P('ep', None, 'tp'), may hold values from -6 to 6
- rec_state: float32 [512, 2048], P('ep', 'tp'), may hold values from -6 to 6
- gate_proj: bfloat16 [2048, 2048], P(None, 'tp'), may hold values from -0.125 to 0.125
- input_proj: bfloat16 [2048, 2048], P(None, 'tp'), may hold values from -0.125 to 0.125
- conv_taps: bfloat16 [4, 2048], P(None, 'tp'), may hold values from -3 to 3
- decay_blocks: bfloat16 [16, 128, 128], P('tp'), may hold values from -0.5 to 0.5
- input_blocks: bfloat16 [16, 128, 128], P('tp'), may hold values from -0.5 to 0.5
- decay_param: float32 [2048], P('tp'), may hold values from 0 to 6
- out_proj: bfloat16 [2048, 2048], P('tp'), may hold values from -0.125 to 0.125
- first_gain: float32 [2048], replicated, may hold values from 0.1 to 1.9
- expert_gate: bfloat16 [4, 2048, 7168], P('ep', None, 'tp'), may hold values from -0.125 to 0.125
- expert_up: bfloat16 [4, 2048, 7168], P('ep', None, 'tp'), may hold values from -0.125 to 0.125
- expert_down: bfloat16 [4, 7168, 2048], P('ep', 'tp'), may hold values from -0.0625 to 0.0625
- routing: int32 [512, 2], P('ep'), may hold values from 0 to 3, all different within a row; in each aligned block of 128 rows (0 to 127, 128 to 255, ...) at most 128 rows name the same one
- route_weight: float32 [512, 2], P('ep'), may hold values from 0.1 to 1
- dense_gate: bfloat16 [2048, 2048], P(None, 'tp'), may hold values from -0.125 to 0.125
- dense_up: bfloat16 [2048, 2048], P(None, 'tp'), may hold values from -0.125 to 0.125
- dense_down: bfloat16 [2048, 2048], P('tp'), may hold values from -0.125 to 0.125
- mix_weight: bfloat16 [2048], replicated, may hold values from -0.125 to 0.125
- second_gain: float32 [2048], P('tp'), may hold values from 0.1 to 1.9
Outputs:
- layer_out: bfloat16 [512, 2048], P('ep', 'tp')
- new_state: float32 [512, 2048], P('ep', 'tp')
- new_conv: bfloat16 [512, 3, 2048], P('ep', None, 'tp')
The draws below stay inside these ranges and needn't reach their ends.
Inputs may be any that keep to these rules, and one draw needn't show every extreme that they name: `routing`: each row names 2 different experts; in each aligned block of 128 rows (the rows of one index of ep) no expert is named by more than 128 rows, a bound that some expert reaches in some block.
All inputs are finite; a program needn't handle non-finite values.
Results may differ from the reference program's by a relative error of at most 0.013.
Values may be sent and summed in bfloat16 or wider, within the bound.
A program may use at most 64 MiB of HBM per device.

```python
import math
import jax
import jax.numpy as jnp
import numpy as np
from jax import lax

D = 2048
DR = 2048
HEADS = 16
BLK = 128
FF = 7168
DFF_D = 2048
TOPK = 2
SEQ_GRP = 128
EXPERTS = 4
CAP = 128
BATCH = 512
N_EP = 4
N_TP = 8


def steps_of(stream_key, extent, cuts, smallest, high):
    factor_of = 1.0
    for axis_at, parts in cuts:
        draws = jax.random.uniform(jax.random.fold_in(jax.random.fold_in(stream_key, 6), axis_at), (parts,), jnp.float32, smallest / len(cuts), high / len(cuts))
        factor_of = factor_of * jnp.repeat(jnp.exp(draws), extent[axis_at] // parts).reshape((-1,) + (1,) * (len(extent) - 1 - axis_at))
    return factor_of


def assign_block(rng, own, number, rows, amount, top, bound, skew):
    sequence = jax.random.permutation(rng, amount)
    packed, usual = shares(amount, rows * top, bound, skew, True), shares(amount, rows * top, bound, skew, False)
    places = jnp.arange(amount)

    def named(sizes, offset_by):
        used = int((sizes > 0).sum())
        fixed = max(1, used // 4)
        passed = fixed + (places - fixed + offset_by * (used - fixed)) % max(1, amount - fixed)
        return jnp.zeros((amount,), jnp.int32).at[sequence[jnp.where(places < fixed, places, passed)]].set(jnp.asarray(sizes, jnp.int32))

    sizes = jnp.where(number % 4 == 0, named(packed, number // 4), named(usual, number - number // 4 - 1))
    mixed = jax.random.permutation(jax.random.fold_in(own, 3), amount)
    giver, taker = mixed[0:amount // 2 * 2:2], mixed[1:amount // 2 * 2:2]
    slack = jnp.minimum(sizes[giver] - 1, bound - sizes[taker]) // 2
    slack = jnp.where((giver == sequence[0]) | (taker == sequence[0]) | (sizes[taker] == 0), 0, jnp.maximum(slack, 0))
    passed = jax.random.randint(jax.random.fold_in(own, 4), (amount // 2,), 0, 1 << 20) % (slack + 1)
    sizes = sizes.at[giver].add(-passed).at[taker].add(passed)
    items = jnp.searchsorted(jnp.cumsum(sizes), jnp.arange(rows * top), side="right").astype(jnp.int32)
    listing = items.reshape(top, rows).T
    listing = listing[jax.random.permutation(jax.random.fold_in(own, 1), rows)]
    offset_by = jax.random.randint(jax.random.fold_in(own, 2), (rows, 1), 0, top)
    return jnp.take_along_axis(listing, (jnp.arange(top)[None, :] + offset_by) % top, axis=1)


def shares(amount, total, bound, lean, full):
    weights = [(1 << 20) // math.isqrt(rank ** lean) + 1 for rank in range(1, amount + 1)]
    largest = bound if full else min(bound, max(-(-total // amount), total * weights[0] // sum(weights)))
    least = 1 if total - largest >= amount - 1 else 0
    given, surplus = [largest] + [least] * (amount - 1), total - largest - least * (amount - 1)
    while surplus > 0:
        free = [i for i in range(1, amount) if given[i] < largest] or [i for i in range(1, amount) if given[i] < bound]
        mass, remaining = sum([weights[i] for i in free]), surplus
        for i in free:
            extra = min(bound - given[i], max(1, remaining * weights[i] // mass), surplus)
            given[i] = given[i] + extra
            surplus = surplus - extra
    return np.array(given)


def normal_values(rng, shape, width, bound, split=(), held_as=jnp.bfloat16):
    factor_of = steps_of(rng, shape, split, -0.22, 0.18) if split else 1.0
    array = jax.random.normal(rng, shape, jnp.float32) * width * factor_of
    return jnp.minimum(jnp.maximum(array, -bound), bound).astype(held_as)


def setup_inputs(seed: int = 0) -> dict:
    key_of = jax.random.split(jax.random.key(seed), 22)
    tokens = normal_values(key_of[0], (BATCH, D), 1.0, 6.0, ((0, 4),))
    conv_state = normal_values(key_of[1], (BATCH, 3, DR), 1.0, 6.0, ((0, 4), (2, 8)))
    rec_state = normal_values(key_of[2], (BATCH, DR), 1.0, 6.0, ((0, 4), (1, 8)), jnp.float32)
    gate_proj = normal_values(key_of[3], (D, DR), D ** -0.5, 0.125, ((1, 8),))
    input_proj = normal_values(key_of[4], (D, DR), D ** -0.5, 0.125, ((1, 8),))
    conv_taps = normal_values(key_of[5], (4, DR), 4 ** -0.5, 3.0, ((1, 8),))
    decay_blocks = normal_values(key_of[6], (HEADS, BLK, BLK), BLK ** -0.5, 0.5, ((0, 8),))
    input_blocks = normal_values(key_of[7], (HEADS, BLK, BLK), BLK ** -0.5, 0.5, ((0, 8),))
    decay_param = jnp.clip(6.0 * jax.random.uniform(key_of[8], (DR,), jnp.float32) ** steps_of(key_of[8], (DR,), ((0, 8),), -0.2, 0.2), 0.0, 6.0)
    out_proj = normal_values(key_of[9], (DR, D), DR ** -0.5, 0.125, ((0, 8),))
    first_gain = jnp.clip(1.0 + 0.18 * jax.random.normal(key_of[10], (D,), jnp.float32), 0.1, 1.9)
    expert_gate = normal_values(key_of[11], (EXPERTS, D, FF), D ** -0.5, 0.125, ((0, 4), (2, 8)))
    expert_up = normal_values(key_of[12], (EXPERTS, D, FF), D ** -0.5, 0.125, ((0, 4), (2, 8)))
    expert_down = normal_values(key_of[13], (EXPERTS, FF, D), FF ** -0.5, 0.0625, ((0, 4), (1, 8)))
    routing_keys = jax.random.split(jax.random.fold_in(key_of[14], 1), BATCH // SEQ_GRP)
    routing_turns = jax.random.permutation(jax.random.fold_in(key_of[14], 3), BATCH // SEQ_GRP)
    routing = jax.vmap(lambda own, number: assign_block(jax.random.fold_in(key_of[14], 2), own, number, SEQ_GRP, EXPERTS, TOPK, CAP, 2))(routing_keys, routing_turns).reshape((BATCH, TOPK))
    route_weight = jnp.clip(jnp.exp(math.log(1.0) - 2.3025851 * jax.random.uniform(key_of[15], (BATCH, TOPK), jnp.float32) ** steps_of(key_of[15], (BATCH, TOPK), ((0, 4),), -0.2, 0.2)), 0.1, 1.0)
    dense_gate = normal_values(key_of[16], (D, DFF_D), D ** -0.5, 0.125, ((1, 8),))
    dense_up = normal_values(key_of[17], (D, DFF_D), D ** -0.5, 0.125, ((1, 8),))
    dense_down = normal_values(key_of[18], (DFF_D, D), DFF_D ** -0.5, 0.125, ((0, 8),))
    mix_weight = normal_values(key_of[19], (D,), D ** -0.5, 0.125)
    second_gain = jnp.clip(1.0 + 0.18 * jax.random.normal(key_of[20], (D,), jnp.float32), 0.1, 1.9)
    return dict(tokens=tokens, conv_state=conv_state, rec_state=rec_state, gate_proj=gate_proj, input_proj=input_proj, conv_taps=conv_taps, decay_blocks=decay_blocks, input_blocks=input_blocks, decay_param=decay_param, out_proj=out_proj, first_gain=first_gain, expert_gate=expert_gate, expert_up=expert_up, expert_down=expert_down, routing=routing, route_weight=route_weight, dense_gate=dense_gate, dense_up=dense_up, dense_down=dense_down, mix_weight=mix_weight, second_gain=second_gain)


ALPHA = 8.0 ** 0.25
RATE_SCALE = 8.0
NORM_EPS = 1e-05

def norm_rows(values, gain_vec):
    centre = values - lax.optimization_barrier(jnp.mean(values, axis=-1, keepdims=True))
    spread = lax.optimization_barrier(jnp.mean(centre * centre, axis=-1, keepdims=True))
    return centre * lax.rsqrt(spread + NORM_EPS) * gain_vec

def split_dot(left, right, pieces):
    rows_count = left.shape[0]
    inner = left.shape[1]
    left_view = left.reshape(rows_count, pieces, inner // pieces).astype(jnp.float32)
    right_view = right.reshape(pieces, inner // pieces, right.shape[1]).astype(jnp.float32)
    partial_value = jnp.einsum('mpk,pkn->pmn', left_view, right_view)
    rounded = lax.optimization_barrier(partial_value.astype(jnp.bfloat16))
    return lax.optimization_barrier(jnp.sum(rounded.astype(jnp.float32), axis=0))

def reference(tokens, conv_state, rec_state, gate_proj, input_proj, conv_taps, decay_blocks, input_blocks, decay_param, out_proj, first_gain, expert_gate, expert_up, expert_down, routing, route_weight, dense_gate, dense_up, dense_down, mix_weight, second_gain):
    count_rows = tokens.shape[0]
    gated = jnp.dot(tokens, gate_proj, preferred_element_type=jnp.float32).astype(jnp.bfloat16)
    inputs = jnp.dot(tokens, input_proj, preferred_element_type=jnp.float32).astype(jnp.bfloat16)
    window = jnp.concatenate([conv_state, inputs[:, None, :]], axis=1)
    convolved = lax.optimization_barrier(jnp.sum(window.astype(jnp.float32) * conv_taps.astype(jnp.float32)[None], axis=1)).astype(jnp.bfloat16)
    heads_view = convolved.reshape(count_rows, HEADS, -1).astype(jnp.float32)
    recur_gate = jax.nn.sigmoid(jnp.einsum('bhi,hij->bhj', heads_view, decay_blocks.astype(jnp.float32))).reshape(count_rows, -1)
    input_gate = jax.nn.sigmoid(jnp.einsum('bhi,hij->bhj', heads_view, input_blocks.astype(jnp.float32))).reshape(count_rows, -1)
    log_decay = -RATE_SCALE * recur_gate * jax.nn.softplus(-decay_param)
    new_state = jnp.exp(log_decay) * rec_state + jnp.sqrt(-jnp.expm1(2.0 * log_decay)) * input_gate * convolved.astype(jnp.float32)
    mixed_rows = (new_state * jax.nn.gelu(gated.astype(jnp.float32), approximate=True)).astype(jnp.bfloat16)
    mixed = split_dot(mixed_rows, out_proj, N_TP)
    normed = norm_rows(ALPHA * tokens.astype(jnp.float32) + mixed, first_gain).astype(jnp.bfloat16)
    experts = expert_gate.shape[0]
    labels = jnp.arange(experts, dtype=jnp.int32)
    weight_table = jnp.zeros((count_rows, experts), jnp.float32)
    routed = jnp.zeros((count_rows, experts), jnp.int32)
    for which in range(TOPK):
        match = routing[:, which][:, None] == labels[None, :]
        weight_table = weight_table + jnp.where(match, route_weight[:, which][:, None], 0.0)
        routed = routed + match.astype(jnp.int32)
    positions = jnp.arange(count_rows, dtype=jnp.int32)
    sort_keys = jnp.where(routed.T > 0, positions[None, :], count_rows + positions[None, :])
    chosen = jnp.argsort(sort_keys, axis=1)[:, :N_EP * CAP].astype(jnp.int32)

    def one_expert(running, members):
        rows_index, weight_col, gate_mat, up_mat, down_mat = members
        rows_data = normed[rows_index]
        gate_val = jnp.dot(rows_data, gate_mat, preferred_element_type=jnp.float32)
        up_val = jnp.dot(rows_data, up_mat, preferred_element_type=jnp.float32)
        hidden = (jax.nn.silu(gate_val) * up_val).astype(jnp.bfloat16)
        result = split_dot(hidden, down_mat, N_TP).astype(jnp.bfloat16)
        running = running.at[rows_index].add(weight_col[rows_index][:, None] * result.astype(jnp.float32))
        return (running, None)
    routed_sum, unused = lax.scan(one_expert, jnp.zeros((count_rows, D), jnp.float32), (chosen, weight_table.T, expert_gate, expert_up, expert_down))
    dense_g = jnp.dot(normed, dense_gate, preferred_element_type=jnp.float32)
    dense_u = jnp.dot(normed, dense_up, preferred_element_type=jnp.float32)
    dense_hidden = (jax.nn.silu(dense_g) * dense_u).astype(jnp.bfloat16)
    dense_out = split_dot(dense_hidden, dense_down, N_TP)
    mix = jax.nn.sigmoid(jnp.dot(normed, mix_weight, preferred_element_type=jnp.float32))
    combined = ALPHA * normed.astype(jnp.float32) + routed_sum + mix[:, None] * dense_out
    layer_out = norm_rows(combined, second_gain).astype(jnp.bfloat16)
    return (layer_out, new_state, window[:, 1:])
```

```python
import functools

import jax
import jax.numpy as jnp
from jax import lax
from jax.experimental import pallas as pl
from jax.experimental.pallas import tpu as pltpu
from jax.sharding import PartitionSpec as P

D = 2048
TOPK = 2


ALPHA = 8.0**0.25
RATE_SCALE = 8.0
NORM_EPS = 1e-05


def norm_rows(values, gain_vec):
    centre = values - jnp.mean(values, axis=-1, keepdims=True)
    spread = jnp.mean(centre * centre, axis=-1, keepdims=True)
    return centre * lax.rsqrt(spread + NORM_EPS) * gain_vec


def on_device_slots(
    tokens,
    conv_state,
    rec_state,
    gate_proj,
    input_proj,
    conv_taps,
    decay_blocks,
    input_blocks,
    decay_param,
    out_proj,
    first_gain,
    expert_gate,
    expert_up,
    expert_down,
    routing,
    route_weight,
    dense_gate,
    dense_up,
    dense_down,
    mix_weight,
    second_gain,
):
    count_rows = tokens.shape[0]
    gated = jnp.dot(tokens, gate_proj, preferred_element_type=jnp.float32).astype(jnp.bfloat16)
    inputs = jnp.dot(tokens, input_proj, preferred_element_type=jnp.float32).astype(jnp.bfloat16)
    window = jnp.concatenate([conv_state, inputs[:, None, :]], axis=1)
    convolved = jnp.sum(
        window.astype(jnp.float32) * conv_taps.astype(jnp.float32)[None], axis=1
    ).astype(jnp.bfloat16)
    local_heads = decay_blocks.shape[0]
    heads_view = convolved.reshape(count_rows, local_heads, -1)
    recur_gate = jax.nn.sigmoid(
        jnp.einsum("bhi,hij->bhj", heads_view, decay_blocks, preferred_element_type=jnp.float32)
    ).reshape(count_rows, -1)
    input_gate = jax.nn.sigmoid(
        jnp.einsum("bhi,hij->bhj", heads_view, input_blocks, preferred_element_type=jnp.float32)
    ).reshape(count_rows, -1)
    log_decay = -RATE_SCALE * recur_gate * jax.nn.softplus(-decay_param)
    new_state = jnp.exp(log_decay) * rec_state + jnp.sqrt(
        -jnp.expm1(2.0 * log_decay)
    ) * input_gate * convolved.astype(jnp.float32)
    mixed_rows = (new_state * jax.nn.gelu(gated.astype(jnp.float32), approximate=True)).astype(
        jnp.bfloat16
    )
    partial_mix = jnp.dot(mixed_rows, out_proj, preferred_element_type=jnp.float32)
    mixed = lax.psum(partial_mix.astype(jnp.bfloat16), "tp").astype(jnp.float32)
    normed = norm_rows(ALPHA * tokens.astype(jnp.float32) + mixed, first_gain).astype(jnp.bfloat16)
    tp_index = lax.axis_index("tp")
    tp_count = lax.axis_size("tp")
    own_width = D // tp_count
    own_normed = lax.dynamic_slice_in_dim(normed, tp_index * own_width, own_width, 1)
    local_experts = expert_gate.shape[0]
    ep_count = lax.axis_size("ep")
    experts = local_experts * ep_count
    capacity = max(2, 2 * count_rows * TOPK // experts)
    flat_routes = routing.reshape(-1)
    labels = jnp.arange(experts, dtype=jnp.int32)
    onehot = (flat_routes[:, None] == labels[None, :]).astype(jnp.int32)
    earlier = jnp.cumsum(onehot, axis=0) - onehot
    slot_index = jnp.sum(earlier * onehot, axis=1)
    target = flat_routes * capacity + slot_index
    placed = (target[:, None] == jnp.arange(experts * capacity, dtype=jnp.int32)[None, :]).astype(
        jnp.bfloat16
    )
    token_slots = jnp.sum(placed.reshape(count_rows, TOPK, experts * capacity), axis=1)
    dispatch = jnp.dot(token_slots.T, normed, preferred_element_type=jnp.float32).astype(
        jnp.bfloat16
    )
    arrived = lax.all_to_all(
        dispatch.reshape(experts, capacity, D), "ep", split_axis=0, concat_axis=1, tiled=True
    )
    gate_val = jnp.einsum("erd,edf->erf", arrived, expert_gate, preferred_element_type=jnp.float32)
    up_val = jnp.einsum("erd,edf->erf", arrived, expert_up, preferred_element_type=jnp.float32)
    hidden = (jax.nn.silu(gate_val) * up_val).astype(jnp.bfloat16)
    partial_out = jnp.einsum(
        "erf,efd->erd", hidden, expert_down, preferred_element_type=jnp.float32
    )
    reduced = lax.psum_scatter(
        partial_out.astype(jnp.bfloat16), "tp", scatter_dimension=2, tiled=True
    )
    returned = lax.all_to_all(reduced, "ep", split_axis=1, concat_axis=0, tiled=True)
    returned = returned.reshape(experts * capacity, own_width)
    picked = jnp.dot(placed, returned, preferred_element_type=jnp.float32).reshape(
        count_rows, TOPK, own_width
    )
    routed_sum = jnp.sum(route_weight[:, :, None] * picked, axis=1)
    dense_g = jnp.dot(normed, dense_gate, preferred_element_type=jnp.float32)
    dense_u = jnp.dot(normed, dense_up, preferred_element_type=jnp.float32)
    dense_hidden = (jax.nn.silu(dense_g) * dense_u).astype(jnp.bfloat16)
    dense_part = jnp.dot(dense_hidden, dense_down, preferred_element_type=jnp.float32)
    dense_out = lax.psum_scatter(
        dense_part.astype(jnp.bfloat16), "tp", scatter_dimension=1, tiled=True
    ).astype(jnp.float32)
    mix = jax.nn.sigmoid(jnp.dot(normed, mix_weight, preferred_element_type=jnp.float32))
    combined = ALPHA * own_normed.astype(jnp.float32) + routed_sum + mix[:, None] * dense_out
    row_total, row_square = lax.psum(
        (jnp.sum(combined, axis=1), jnp.sum(combined * combined, axis=1)), "tp"
    )
    row_mean = row_total / D
    row_var = row_square / D - row_mean * row_mean
    layer_out = (
        (combined - row_mean[:, None]) * lax.rsqrt(row_var[:, None] + NORM_EPS) * second_gain
    ).astype(jnp.bfloat16)
    return (layer_out, new_state, window[:, 1:])


MESH = pl.DeviceIdType.MESH


def xor(left, right, count):
    total, bit = 0, 1
    while bit < count:
        lbit, rbit = (left // bit) % 2, (right // bit) % 2
        total = total + bit * (lbit + rbit - 2 * lbit * rbit)
        bit *= 2
    return total


def block_kernel(
    n_ep,
    n_tp,
    tokens_hbm,
    conv_ref,
    state_ref,
    gproj_hbm,
    iproj_hbm,
    taps_ref,
    dblk_ref,
    iblk_ref,
    dparam_ref,
    oproj_hbm,
    fgain_ref,
    eg_hbm,
    eu_hbm,
    ed_hbm,
    routing_ref,
    rweight_ref,
    dg_hbm,
    du_hbm,
    dd_hbm,
    mixw_ref,
    sgain_ref,
    out_ref,
    nstate_ref,
    nconv_ref,
    tok,
    gproj,
    iproj,
    oproj,
    eg,
    eu,
    ed,
    dg,
    du,
    dd,
    pmix,
    pmix_in,
    smix,
    smix_in,
    xall,
    hid,
    dhid,
    wtab,
    part,
    part_in,
    psum,
    ret_in,
    zout,
    zin,
    oout,
    oin,
    wsem,
    bpair,
    bz_s,
    bz_r,
    agz_s,
    agz_r,
    age_s,
    age_r,
    sib_s,
    sib_r,
    rp_s,
    rp_r,
    re_s,
    re_r,
    rz_s,
    rz_r,
    o_s,
    o_r,
):
    f32, bf16 = jnp.float32, jnp.bfloat16
    e, t = lax.axis_index("ep"), lax.axis_index("tp")
    n_z = n_tp // 2
    c, k = t % 2, t // 2
    other = 1 - c
    sibling = 2 * k + other
    rr, width = tok.shape[1], tok.shape[2]
    rows = n_tp * rr
    wide = min(512, width)

    loads = [
        pltpu.make_async_copy(a, b, wsem.at[i])
        for i, (a, b) in enumerate(
            [
                (tokens_hbm, tok),
                (iproj_hbm, iproj),
                (gproj_hbm, gproj),
                (oproj_hbm, oproj),
                (dg_hbm, dg),
                (du_hbm, du),
                (dd_hbm, dd),
                (eg_hbm, eg),
                (eu_hbm, eu),
                (ed_hbm, ed),
            ]
        )
    ]
    for load in loads:
        load.start()

    barrier = pltpu.get_barrier_semaphore()
    for d in range(1, n_tp):
        pl.semaphore_signal(barrier, inc=1, device_id=(e, xor(t, d, n_tp)), device_id_type=MESH)
    for d in range(1, n_ep):
        pl.semaphore_signal(barrier, inc=1, device_id=(xor(e, d, n_ep), t), device_id_type=MESH)

    def remote(src, dst, send, recv, ep, tp):
        return pltpu.make_async_remote_copy(
            src_ref=src, dst_ref=dst, send_sem=send, recv_sem=recv,
            device_id=(ep, tp), device_id_type=MESH,
        )

    route, rweight = routing_ref[...], rweight_ref[...]
    for s in range(n_ep):
        col = jnp.zeros((rows, 1), f32)
        for j in range(TOPK):
            col = col + jnp.where(route[:, j : j + 1] == s, rweight[:, j : j + 1], 0.0)
        wtab[s] = jnp.broadcast_to(col, (rows, 128)).reshape(n_tp, rr, 128)

    loads[0].wait()
    loads[1].wait()
    tokens = tok[...].reshape(rows, width)
    inputs = jnp.dot(tokens, iproj[...], preferred_element_type=f32).astype(bf16)
    taps = taps_ref[...].astype(f32)
    conv = inputs.astype(f32) * taps[3:4]
    for j in range(3):
        conv = conv + conv_ref[j].astype(f32) * taps[j : j + 1]
    nconv_ref[0] = conv_ref[1]
    nconv_ref[1] = conv_ref[2]
    nconv_ref[2] = inputs
    conv = conv.astype(bf16)
    heads, blk = dblk_ref.shape[0], dblk_ref.shape[1]

    def by_head(ref):
        parts = [
            jnp.dot(conv[:, h * blk : (h + 1) * blk], ref[h], preferred_element_type=f32)
            for h in range(heads)
        ]
        return jax.nn.sigmoid(jnp.concatenate(parts, axis=1))

    recur_gate, input_gate = by_head(dblk_ref), by_head(iblk_ref)
    neg = -dparam_ref[...]
    soft = jnp.maximum(neg, 0.0) + jnp.log1p(jnp.exp(-jnp.abs(neg)))
    log_decay = -RATE_SCALE * recur_gate * soft
    decay = jnp.exp(log_decay)
    new_state = decay * state_ref[...] + jnp.sqrt(
        -jnp.tanh(log_decay) * (decay * decay + 1.0)
    ) * input_gate * conv.astype(f32)
    nstate_ref[...] = new_state
    loads[2].wait()
    gated = jnp.dot(tokens, gproj[...], preferred_element_type=f32).astype(bf16).astype(f32)
    mixed = (new_state * jax.nn.gelu(gated, approximate=True)).astype(bf16)
    loads[3].wait()
    for n0 in range(0, width, wide):
        val = jnp.dot(mixed, oproj[:, n0 : n0 + wide], preferred_element_type=f32).astype(bf16)
        for j in range(n_tp):
            pmix[j % 2, j // 2, :, n0 : n0 + wide] = val[j * rr : (j + 1) * rr]
    pl.semaphore_wait(barrier, n_tp - 1 + n_ep - 1)

    copy = remote(pmix.at[other], pmix_in, bpair.at[0], bpair.at[1], e, sibling)
    copy.start()
    copy.wait_recv()
    zcopies = []
    for d in range(1, n_z):
        kk = xor(k, d, n_z)
        smix[d] = (pmix[c, kk].astype(f32) + pmix_in[kk].astype(f32)).astype(bf16)
        zc = remote(smix.at[d], smix_in.at[d], bz_s.at[d], bz_r.at[d], e, 2 * kk + c)
        zc.start()
        zcopies.append(zc)
    mix_rows = pmix[c, k].astype(f32) + pmix_in[k].astype(f32)
    mix_rows = mix_rows + ALPHA * tok[t].astype(f32)
    for d in range(1, n_z):
        zcopies[d - 1].wait_recv()
        mix_rows = mix_rows + smix_in[d].astype(f32)
    normed = norm_rows(mix_rows, fgain_ref[...]).astype(bf16)
    xall[e, c, k] = normed

    def block(dge, dk):
        return xall.at[xor(e, dge, n_ep), c, xor(k, dk, n_z)]

    agz, age, sib = [], {}, {}
    own = xall.at[e, c, k]
    for d in range(1, n_z):
        zc = remote(own, own, agz_s.at[d], agz_r.at[d], e, 2 * xor(k, d, n_z) + c)
        zc.start()
        agz.append(zc)

    def to_ep(dge, dk):
        src = xall.at[e, c, xor(k, dk, n_z)]
        ec = remote(src, src, age_s.at[dge, dk], age_r.at[dge, dk], xor(e, dge, n_ep), t)
        ec.start()
        age[dge, dk] = ec

    single = [d for d in range(1, n_ep) if d & (d - 1) == 0]
    double = [d for d in range(1, n_ep) if d & (d - 1)]
    for dge in single:
        to_ep(dge, 0)
    for d in range(1, n_z):
        agz[d - 1].wait_recv()
        for dge in single:
            to_ep(dge, d)
    for d in range(n_z):
        for dge in double:
            to_ep(dge, d)

    def to_sibling(dge):
        src = xall.at[xor(e, dge, n_ep), c]
        return remote(src, src, sib_s.at[dge], sib_r.at[dge], e, sibling)

    def from_ep(dge):
        for dk in range(n_z):
            dst = xall.at[xor(e, dge, n_ep), c, xor(k, dk, n_z)]
            remote(dst, dst, age_s.at[dge, dk], age_r.at[dge, dk], xor(e, dge, n_ep), t).wait_recv()

    to_sibling(0).start()
    to_sibling(0).wait_recv()

    ff = eg.shape[1]
    rows_own = xall[e].reshape(rows, width)
    for i in (4, 5):
        loads[i].wait()
    dhid[...] = (
        jax.nn.silu(jnp.dot(rows_own, dg[...], preferred_element_type=f32))
        * jnp.dot(rows_own, du[...], preferred_element_type=f32)
    ).astype(bf16)
    mix = jax.nn.sigmoid(
        jnp.sum(rows_own.astype(f32) * mixw_ref[...].astype(f32), axis=1, keepdims=True)
    )
    for i in (6, 7, 8, 9):
        loads[i].wait()

    def hidden(g):
        x = xall[g].reshape(rows, width)
        for f0 in range(0, ff, 256):
            f1 = min(ff, f0 + 256)
            gate_val = jnp.dot(x, eg[:, f0:f1], preferred_element_type=f32)
            up_val = jnp.dot(x, eu[:, f0:f1], preferred_element_type=f32)
            hid[:, f0:f1] = (jax.nn.silu(gate_val) * up_val).astype(bf16)

    def to_pair(dge):
        return remote(
            part.at[dge, other], part_in.at[dge], rp_s.at[dge], rp_r.at[dge], e, sibling
        )

    def to_owner(dge):
        return remote(
            psum.at[dge], ret_in.at[dge], re_s.at[dge], re_r.at[dge], xor(e, dge, n_ep), t
        )

    hidden(e)
    weights = jnp.concatenate(
        [wtab[e, 2 * kk + cc][:, :1] for cc in range(2) for kk in range(n_z)], axis=0
    )
    for n0 in range(0, width, wide):
        val = weights * jnp.dot(hid[...], ed[:, n0 : n0 + wide], preferred_element_type=f32)
        val = val + mix * jnp.dot(dhid[...], dd[:, n0 : n0 + wide], preferred_element_type=f32)
        part[0, :, :, :, n0 : n0 + wide] = val.astype(bf16).reshape(2, n_z, rr, wide)
    to_pair(0).start()

    def finish(dge):
        to_pair(dge).wait_recv()
        for kk in range(n_z):
            psum[dge, kk] = (
                part[dge, c, kk].astype(f32) + part_in[dge, kk].astype(f32)
            ).astype(bf16)
        to_owner(dge).start()

    def step(dge, carry):
        from_ep(dge)
        to_sibling(dge).start()
        to_sibling(dge).wait_recv()
        hidden(xor(e, dge, n_ep))
        for n0 in range(0, width, wide):
            val = jnp.dot(hid[...], ed[:, n0 : n0 + wide], preferred_element_type=f32)
            part[dge, :, :, :, n0 : n0 + wide] = val.astype(bf16).reshape(2, n_z, rr, wide)
        to_pair(dge).start()
        finish(dge)
        return carry

    lax.fori_loop(1, n_ep, step, 0)

    to_pair(0).wait_recv()
    for dge in range(1, n_ep):
        to_owner(dge).wait_recv()

    def combine(kk):
        total = part[0, c, kk].astype(f32) + part_in[0, kk].astype(f32)
        for dge in range(1, n_ep):
            weight = wtab[xor(e, dge, n_ep), 2 * kk + c][:, :1]
            total = total + weight * ret_in[dge, kk].astype(f32)
        return total

    zcopies2 = []
    for d in range(1, n_z):
        kk = xor(k, d, n_z)
        zout[d] = combine(kk).astype(bf16)
        zc = remote(zout.at[d], zin.at[d], rz_s.at[d], rz_r.at[d], e, 2 * kk + c)
        zc.start()
        zcopies2.append(zc)
    total = combine(k) + ALPHA * xall[e, c, k].astype(f32)
    for d in range(1, n_z):
        zcopies2[d - 1].wait_recv()
        total = total + zin[d].astype(f32)
    final = norm_rows(total, 1.0)
    cols = width // n_tp
    for j in range(n_tp):
        oout[j] = final[:, j * cols : (j + 1) * cols]
    ocopies = []
    for d in range(1, n_tp):
        peer = xor(t, d, n_tp)
        oc = remote(oout.at[peer], oin.at[t], o_s.at[d], o_r.at[d], e, peer)
        oc.start()
        ocopies.append(oc)
    oin[t] = oout[t]
    for d in range(1, n_tp):
        peer = xor(t, d, n_tp)
        remote(oout.at[peer], oin.at[peer], o_s.at[d], o_r.at[d], e, peer).wait_recv()
    out_ref[...] = (oin[...].reshape(rows, cols) * sgain_ref[...]).astype(bf16)

    copy.wait_send()
    for group in (zcopies, agz, zcopies2, ocopies):
        for each in group:
            each.wait_send()
    for each in age.values():
        each.wait_send()
    for dge in range(n_ep):
        to_sibling(dge).wait_send()
        to_pair(dge).wait_send()
        if dge:
            to_owner(dge).wait_send()


def on_device(*args):
    tokens, routing, expert_gate = args[0], args[14], args[11]
    rows, width = tokens.shape
    n_ep, n_tp = lax.axis_size("ep"), lax.axis_size("tp")
    experts = expert_gate.shape[0] * n_ep
    capacity = max(2, 2 * rows * TOPK // experts)
    if capacity < rows or expert_gate.shape[0] != 1 or n_ep & (n_ep - 1) or n_tp & (n_tp - 1):
        return on_device_slots(*args)
    rr, n_z = rows // n_tp, n_tp // 2
    own, ff = args[3].shape[1], expert_gate.shape[2]
    bf16, f32 = jnp.bfloat16, jnp.float32
    operands = list(args)
    operands[0] = tokens.reshape(n_tp, rr, width)
    operands[1] = jnp.transpose(args[1], (1, 0, 2))
    for i in (8, 10, 19, 20):
        operands[i] = args[i].reshape(1, -1)
    for i in (11, 12, 13):
        operands[i] = args[i][0]
    in_hbm = (0, 3, 4, 9, 11, 12, 13, 16, 17, 18)
    vmem = pl.BlockSpec(memory_space=pltpu.VMEM)
    dma = pltpu.SemaphoreType.DMA
    layer_out, new_state, new_conv = pl.pallas_call(
        functools.partial(block_kernel, n_ep, n_tp),
        out_shape=(
            jax.ShapeDtypeStruct((rows, own), bf16),
            jax.ShapeDtypeStruct((rows, own), f32),
            jax.ShapeDtypeStruct((3, rows, own), bf16),
        ),
        in_specs=[
            pl.BlockSpec(memory_space=pl.ANY) if i in in_hbm else vmem
            for i in range(len(operands))
        ],
        out_specs=(vmem, vmem, vmem),
        scratch_shapes=[
            pltpu.VMEM((n_tp, rr, width), bf16),
            pltpu.VMEM((width, own), bf16),
            pltpu.VMEM((width, own), bf16),
            pltpu.VMEM((own, width), bf16),
            pltpu.VMEM((width, ff), bf16),
            pltpu.VMEM((width, ff), bf16),
            pltpu.VMEM((ff, width), bf16),
            pltpu.VMEM(args[16].shape, bf16),
            pltpu.VMEM(args[17].shape, bf16),
            pltpu.VMEM(args[18].shape, bf16),
            pltpu.VMEM((2, n_z, rr, width), bf16),
            pltpu.VMEM((n_z, rr, width), bf16),
            pltpu.VMEM((n_z, rr, width), bf16),
            pltpu.VMEM((n_z, rr, width), bf16),
            pltpu.VMEM((n_ep, 2, n_z, rr, width), bf16),
            pltpu.VMEM((rows, ff), bf16),
            pltpu.VMEM((rows, args[16].shape[1]), bf16),
            pltpu.VMEM((n_ep, n_tp, rr, 128), f32),
            pltpu.VMEM((n_ep, 2, n_z, rr, width), bf16),
            pltpu.VMEM((n_ep, n_z, rr, width), bf16),
            pltpu.VMEM((n_ep, n_z, rr, width), bf16),
            pltpu.VMEM((n_ep, n_z, rr, width), bf16),
            pltpu.VMEM((n_z, rr, width), bf16),
            pltpu.VMEM((n_z, rr, width), bf16),
            pltpu.VMEM((n_tp, rr, width // n_tp), f32),
            pltpu.VMEM((n_tp, rr, width // n_tp), f32),
            dma((len(in_hbm),)),
            dma((2,)),
            dma((n_z,)),
            dma((n_z,)),
            dma((n_z,)),
            dma((n_z,)),
            dma((n_ep, n_z)),
            dma((n_ep, n_z)),
            dma((n_ep,)),
            dma((n_ep,)),
            dma((n_ep,)),
            dma((n_ep,)),
            dma((n_ep,)),
            dma((n_ep,)),
            dma((n_z,)),
            dma((n_z,)),
            dma((n_tp,)),
            dma((n_tp,)),
        ],
        compiler_params=pltpu.CompilerParams(
            collective_id=0, has_side_effects=True, vmem_limit_bytes=56 * 2**20
        ),
    )(*operands)
    return layer_out, new_state, jnp.transpose(new_conv, (1, 0, 2))


def solution(mesh):
    return jax.shard_map(
        on_device,
        mesh=mesh,
        in_specs=(
            P("ep", None),
            P("ep", None, "tp"),
            P("ep", "tp"),
            P(None, "tp"),
            P(None, "tp"),
            P(None, "tp"),
            P("tp", None, None),
            P("tp", None, None),
            P("tp"),
            P("tp", None),
            P(),
            P("ep", None, "tp"),
            P("ep", None, "tp"),
            P("ep", "tp", None),
            P("ep", None),
            P("ep", None),
            P(None, "tp"),
            P(None, "tp"),
            P("tp", None),
            P(),
            P("tp"),
        ),
        out_specs=(P("ep", "tp"), P("ep", "tp"), P("ep", None, "tp")),
        check_vma=False,
    )
```

```python
import functools

import jax
import jax.numpy as jnp
from jax import lax
from jax.experimental import pallas as pl
from jax.experimental.pallas import tpu as pltpu
from jax.sharding import PartitionSpec as P

D = 2048
TOPK = 2


ALPHA = 8.0**0.25
RATE_SCALE = 8.0
NORM_EPS = 1e-05


def norm_rows(values, gain_vec):
    centre = values - jnp.mean(values, axis=-1, keepdims=True)
    spread = jnp.mean(centre * centre, axis=-1, keepdims=True)
    return centre * lax.rsqrt(spread + NORM_EPS) * gain_vec


def on_device_slots(
    tokens,
    conv_state,
    rec_state,
    gate_proj,
    input_proj,
    conv_taps,
    decay_blocks,
    input_blocks,
    decay_param,
    out_proj,
    first_gain,
    expert_gate,
    expert_up,
    expert_down,
    routing,
    route_weight,
    dense_gate,
    dense_up,
    dense_down,
    mix_weight,
    second_gain,
):
    count_rows = tokens.shape[0]
    gated = jnp.dot(tokens, gate_proj, preferred_element_type=jnp.float32).astype(jnp.bfloat16)
    inputs = jnp.dot(tokens, input_proj, preferred_element_type=jnp.float32).astype(jnp.bfloat16)
    window = jnp.concatenate([conv_state, inputs[:, None, :]], axis=1)
    convolved = jnp.sum(
        window.astype(jnp.float32) * conv_taps.astype(jnp.float32)[None], axis=1
    ).astype(jnp.bfloat16)
    local_heads = decay_blocks.shape[0]
    heads_view = convolved.reshape(count_rows, local_heads, -1)
    recur_gate = jax.nn.sigmoid(
        jnp.einsum("bhi,hij->bhj", heads_view, decay_blocks, preferred_element_type=jnp.float32)
    ).reshape(count_rows, -1)
    input_gate = jax.nn.sigmoid(
        jnp.einsum("bhi,hij->bhj", heads_view, input_blocks, preferred_element_type=jnp.float32)
    ).reshape(count_rows, -1)
    log_decay = -RATE_SCALE * recur_gate * jax.nn.softplus(-decay_param)
    new_state = jnp.exp(log_decay) * rec_state + jnp.sqrt(
        -jnp.expm1(2.0 * log_decay)
    ) * input_gate * convolved.astype(jnp.float32)
    mixed_rows = (new_state * jax.nn.gelu(gated.astype(jnp.float32), approximate=True)).astype(
        jnp.bfloat16
    )
    partial_mix = jnp.dot(mixed_rows, out_proj, preferred_element_type=jnp.float32)
    mixed = lax.psum(partial_mix.astype(jnp.bfloat16), "tp").astype(jnp.float32)
    normed = norm_rows(ALPHA * tokens.astype(jnp.float32) + mixed, first_gain).astype(jnp.bfloat16)
    tp_index = lax.axis_index("tp")
    tp_count = lax.axis_size("tp")
    own_width = D // tp_count
    own_normed = lax.dynamic_slice_in_dim(normed, tp_index * own_width, own_width, 1)
    local_experts = expert_gate.shape[0]
    ep_count = lax.axis_size("ep")
    experts = local_experts * ep_count
    capacity = max(2, 2 * count_rows * TOPK // experts)
    flat_routes = routing.reshape(-1)
    labels = jnp.arange(experts, dtype=jnp.int32)
    onehot = (flat_routes[:, None] == labels[None, :]).astype(jnp.int32)
    earlier = jnp.cumsum(onehot, axis=0) - onehot
    slot_index = jnp.sum(earlier * onehot, axis=1)
    target = flat_routes * capacity + slot_index
    placed = (target[:, None] == jnp.arange(experts * capacity, dtype=jnp.int32)[None, :]).astype(
        jnp.bfloat16
    )
    token_slots = jnp.sum(placed.reshape(count_rows, TOPK, experts * capacity), axis=1)
    dispatch = jnp.dot(token_slots.T, normed, preferred_element_type=jnp.float32).astype(
        jnp.bfloat16
    )
    arrived = lax.all_to_all(
        dispatch.reshape(experts, capacity, D), "ep", split_axis=0, concat_axis=1, tiled=True
    )
    gate_val = jnp.einsum("erd,edf->erf", arrived, expert_gate, preferred_element_type=jnp.float32)
    up_val = jnp.einsum("erd,edf->erf", arrived, expert_up, preferred_element_type=jnp.float32)
    hidden = (jax.nn.silu(gate_val) * up_val).astype(jnp.bfloat16)
    partial_out = jnp.einsum(
        "erf,efd->erd", hidden, expert_down, preferred_element_type=jnp.float32
    )
    reduced = lax.psum_scatter(
        partial_out.astype(jnp.bfloat16), "tp", scatter_dimension=2, tiled=True
    )
    returned = lax.all_to_all(reduced, "ep", split_axis=1, concat_axis=0, tiled=True)
    returned = returned.reshape(experts * capacity, own_width)
    picked = jnp.dot(placed, returned, preferred_element_type=jnp.float32).reshape(
        count_rows, TOPK, own_width
    )
    routed_sum = jnp.sum(route_weight[:, :, None] * picked, axis=1)
    dense_g = jnp.dot(normed, dense_gate, preferred_element_type=jnp.float32)
    dense_u = jnp.dot(normed, dense_up, preferred_element_type=jnp.float32)
    dense_hidden = (jax.nn.silu(dense_g) * dense_u).astype(jnp.bfloat16)
    dense_part = jnp.dot(dense_hidden, dense_down, preferred_element_type=jnp.float32)
    dense_out = lax.psum_scatter(
        dense_part.astype(jnp.bfloat16), "tp", scatter_dimension=1, tiled=True
    ).astype(jnp.float32)
    mix = jax.nn.sigmoid(jnp.dot(normed, mix_weight, preferred_element_type=jnp.float32))
    combined = ALPHA * own_normed.astype(jnp.float32) + routed_sum + mix[:, None] * dense_out
    row_total, row_square = lax.psum(
        (jnp.sum(combined, axis=1), jnp.sum(combined * combined, axis=1)), "tp"
    )
    row_mean = row_total / D
    row_var = row_square / D - row_mean * row_mean
    layer_out = (
        (combined - row_mean[:, None]) * lax.rsqrt(row_var[:, None] + NORM_EPS) * second_gain
    ).astype(jnp.bfloat16)
    return (layer_out, new_state, window[:, 1:])


MESH = pl.DeviceIdType.MESH


def xor(left, right, count):
    total, bit = 0, 1
    while bit < count:
        lbit, rbit = (left // bit) % 2, (right // bit) % 2
        total = total + bit * (lbit + rbit - 2 * lbit * rbit)
        bit *= 2
    return total


def block_kernel(
    n_ep,
    n_tp,
    tokens_hbm,
    conv_ref,
    state_ref,
    gproj_hbm,
    iproj_hbm,
    taps_ref,
    dblk_ref,
    iblk_ref,
    dparam_ref,
    oproj_hbm,
    fgain_ref,
    eg_hbm,
    eu_hbm,
    ed_hbm,
    routing_ref,
    rweight_ref,
    dg_hbm,
    du_hbm,
    dd_hbm,
    mixw_ref,
    oin,
    nstate_ref,
    nconv_ref,
    tok,
    gproj,
    iproj,
    oproj,
    eg,
    eu,
    ed,
    dg,
    du,
    dd,
    pmix,
    pmix_in,
    smix,
    smix_in,
    xall,
    hid,
    dhid,
    part,
    part_in,
    psum,
    diag_in,
    ret_in,
    zout,
    zin,
    oout,
    wsend,
    wrecv,
    wsem,
    bpair,
    bz_s,
    bz_r,
    agz_s,
    agz_r,
    age_s,
    age_r,
    sib_s,
    sib_r,
    rp_s,
    rp_r,
    re_s,
    re_r,
    rd_s,
    rd_r,
    w_s,
    w_r,
    rz_s,
    rz_r,
    o_s,
    o_r,
):
    f32, bf16 = jnp.float32, jnp.bfloat16
    e, t = lax.axis_index("ep"), lax.axis_index("tp")
    n_z = n_tp // 2
    c, k = t % 2, t // 2
    other = 1 - c
    sibling = 2 * k + other
    rr, width = tok.shape[1], tok.shape[2]
    rows = n_tp * rr
    wide = min(512, width)

    loads = [
        pltpu.make_async_copy(a, b, wsem.at[i])
        for i, (a, b) in enumerate(
            [
                (tokens_hbm, tok),
                (iproj_hbm, iproj),
                (gproj_hbm, gproj),
                (oproj_hbm, oproj),
                (dg_hbm, dg),
                (du_hbm, du),
                (dd_hbm, dd),
                (eg_hbm, eg),
                (eu_hbm, eu),
                (ed_hbm, ed),
            ]
        )
    ]
    for load in loads[:4]:
        load.start()

    barrier = pltpu.get_barrier_semaphore()
    for d in range(1, n_tp):
        pl.semaphore_signal(barrier, inc=1, device_id=(e, xor(t, d, n_tp)), device_id_type=MESH)
    for d in range(1, n_ep):
        pl.semaphore_signal(barrier, inc=1, device_id=(xor(e, d, n_ep), t), device_id_type=MESH)

    def remote(src, dst, send, recv, ep, tp):
        return pltpu.make_async_remote_copy(
            src_ref=src, dst_ref=dst, send_sem=send, recv_sem=recv,
            device_id=(ep, tp), device_id_type=MESH,
        )

    route, rweight = routing_ref[...], rweight_ref[...]
    for d in range(n_ep):
        row = jnp.zeros((1, rows), f32)
        for j in range(TOPK):
            row = row + jnp.where(
                route[j : j + 1] == xor(e, d, n_ep), rweight[j : j + 1], 0.0
            )
        wsend[d] = jnp.broadcast_to(row, (8, rows))

    loads[0].wait()
    loads[1].wait()
    tokens = tok[...].reshape(rows, width)
    inputs = jnp.dot(tokens, iproj[...], preferred_element_type=f32).astype(bf16)
    taps = taps_ref[...].astype(f32)
    conv = inputs.astype(f32) * taps[3:4]
    for j in range(3):
        conv = conv + conv_ref[j].astype(f32) * taps[j : j + 1]
    nconv_ref[0] = conv_ref[1]
    nconv_ref[1] = conv_ref[2]
    nconv_ref[2] = inputs
    conv = conv.astype(bf16)
    heads, blk = dblk_ref.shape[0], dblk_ref.shape[1]

    def by_head(ref):
        parts = [
            jnp.dot(conv[:, h * blk : (h + 1) * blk], ref[h], preferred_element_type=f32)
            for h in range(heads)
        ]
        return jax.nn.sigmoid(jnp.concatenate(parts, axis=1))

    recur_gate, input_gate = by_head(dblk_ref), by_head(iblk_ref)
    neg = -dparam_ref[...]
    soft = jnp.maximum(neg, 0.0) + jnp.log1p(jnp.exp(-jnp.abs(neg)))
    log_decay = -RATE_SCALE * recur_gate * soft
    decay = jnp.exp(log_decay)
    new_state = decay * state_ref[...] + jnp.sqrt(
        -jnp.tanh(log_decay) * (decay * decay + 1.0)
    ) * input_gate * conv.astype(f32)
    nstate_ref[...] = new_state
    loads[2].wait()
    loads[3].wait()
    for load in loads[4:]:
        load.start()
    gated = jnp.dot(tokens, gproj[...], preferred_element_type=f32).astype(bf16).astype(f32)
    mixed = (new_state * jax.nn.gelu(gated, approximate=True)).astype(bf16)
    for n0 in range(0, width, wide):
        val = jnp.dot(mixed, oproj[:, n0 : n0 + wide], preferred_element_type=f32).astype(bf16)
        for j in range(n_tp):
            pmix[j % 2, j // 2, :, n0 : n0 + wide] = val[j * rr : (j + 1) * rr]
    pl.semaphore_wait(barrier, n_tp - 1 + n_ep - 1)

    copy = remote(pmix.at[other], pmix_in, bpair.at[0], bpair.at[1], e, sibling)
    copy.start()
    wcopies = [None]
    for d in range(1, n_ep):
        wc = remote(wsend.at[d], wrecv.at[d], w_s.at[d], w_r.at[d], xor(e, d, n_ep), t)
        wc.start()
        wcopies.append(wc)
    copy.wait_recv()
    zcopies = []
    for d in range(1, n_z):
        kk = xor(k, d, n_z)
        smix[d] = (pmix[c, kk].astype(f32) + pmix_in[kk].astype(f32)).astype(bf16)
        zc = remote(smix.at[d], smix_in.at[d], bz_s.at[d], bz_r.at[d], e, 2 * kk + c)
        zc.start()
        zcopies.append(zc)
    mix_rows = pmix[c, k].astype(f32) + pmix_in[k].astype(f32)
    mix_rows = mix_rows + ALPHA * tok[t].astype(f32)
    for d in range(1, n_z):
        zcopies[d - 1].wait_recv()
        mix_rows = mix_rows + smix_in[d].astype(f32)
    normed = norm_rows(mix_rows, fgain_ref[...]).astype(bf16)
    xall[e, c, k] = normed

    agz, age, sib, pair = [], {}, {}, {}
    half = n_z // 2

    def slot(dge, dk):
        return xall.at[xor(e, dge, n_ep), c, xor(k, dk, n_z)]

    for d in range(1, n_z):
        zc = remote(
            slot(0, 0), slot(0, 0), agz_s.at[d], agz_r.at[d], e, 2 * xor(k, d, n_z) + c
        )
        zc.start()
        agz.append(zc)

    def to_ep(dge, dk, origin=0):
        src = slot(origin, dk)
        at = dge ^ origin
        ec = remote(src, src, age_s.at[at, dk], age_r.at[at, dk], xor(e, dge, n_ep), t)
        ec.start()
        age[at, dk] = ec

    def to_sibling(dge):
        src = xall.at[xor(e, dge, n_ep), c]
        sib[dge] = remote(src, src, sib_s.at[dge], sib_r.at[dge], e, sibling)
        sib[dge].start()

    def forward(dk):
        age[1, dk].wait_recv()
        age[2, dk].wait_recv()
        if dk < half:
            to_ep(2, dk, 1)
        else:
            to_ep(1, dk, 2)

    for dk in range(n_z):
        if dk:
            agz[dk - 1].wait_recv()
        to_ep(1, dk)
        to_ep(2, dk)
    to_sibling(0)

    ff = eg.shape[1]
    forward(0)
    sib[0].wait_recv()
    for i in (4, 5):
        loads[i].wait()
    rows_own = xall[e].reshape(rows, width)
    dhid[...] = (
        jax.nn.silu(jnp.dot(rows_own, dg[...], preferred_element_type=f32))
        * jnp.dot(rows_own, du[...], preferred_element_type=f32)
    ).astype(bf16)
    for dk in range(1, n_z):
        forward(dk)
    to_sibling(1)
    to_sibling(2)
    mix = jax.nn.sigmoid(
        jnp.sum(
            rows_own.astype(f32) * mixw_ref[...].astype(f32).reshape(1, width),
            axis=1,
            keepdims=True,
        )
    )
    for i in (6, 7, 8, 9):
        loads[i].wait()

    def hidden(dge):
        x = xall[xor(e, dge, n_ep)].reshape(rows, width)
        for f0 in range(0, ff, 256):
            f1 = min(ff, f0 + 256)
            gate_val = jnp.dot(x, eg[:, f0:f1], preferred_element_type=f32)
            up_val = jnp.dot(x, eu[:, f0:f1], preferred_element_type=f32)
            hid[:, f0:f1] = (jax.nn.silu(gate_val) * up_val).astype(bf16)

    def down(dge):
        row = (wrecv if dge else wsend)[dge][:1]
        across = lax.broadcasted_iota(jnp.int32, (rows, rows), 0)
        along = lax.broadcasted_iota(jnp.int32, (rows, rows), 1)
        col = jnp.sum(jnp.where(across == along, row, 0.0), axis=1, keepdims=True)
        weights = jnp.concatenate(
            [col[j * rr : (j + 1) * rr] for cc in range(2) for j in range(cc, n_tp, 2)], axis=0
        )
        for n0 in range(0, width, wide):
            cut = slice(n0, n0 + wide)
            val = weights * jnp.dot(hid[...], ed[:, cut], preferred_element_type=f32)
            if dge == 0:
                val = val + mix * jnp.dot(dhid[...], dd[:, cut], preferred_element_type=f32)
            part[dge, :, :, :, cut] = val.astype(bf16).reshape(2, n_z, rr, wide)
        pair[dge] = remote(
            part.at[dge, other], part_in.at[dge], rp_s.at[dge], rp_r.at[dge], e, sibling
        )
        pair[dge].start()

    def chip_sum(dge, kk):
        return part[dge, c, kk].astype(f32) + part_in[dge, kk].astype(f32)

    blocks = {1: (0, half), 2: (half, 0)}
    sends = []

    def send(src, dst, sems, at, dge):
        rc = remote(src, dst, sems[0].at[at], sems[1].at[at], xor(e, dge, n_ep), t)
        rc.start()
        sends.append(rc)
        return rc

    returns, diagonal = [], {}

    def finish(dge):
        pair[dge].wait_recv()
        if dge == 3:
            for to, b0 in ((1, 0), (2, half)):
                for kk in range(b0, b0 + half):
                    psum[3, kk] = chip_sum(3, kk).astype(bf16)
                cut = pl.ds(b0, half)
                diagonal[to] = send(
                    psum.at[3, cut], diag_in.at[cut], (rd_s, rd_r), to, to
                )
            return
        b0 = blocks[dge][0]
        for kk in range(b0, b0 + half):
            psum[dge, kk] = chip_sum(dge, kk).astype(bf16)
        cut = pl.ds(b0, half)
        returns.append(
            send(psum.at[dge, cut], ret_in.at[dge, cut], (re_s, re_r), 2 * dge, dge)
        )

    def finish_late(dge):
        diagonal[3 - dge].wait_recv()
        b0 = blocks[dge][1]
        for kk in range(b0, b0 + half):
            psum[dge, kk] = (chip_sum(dge, kk) + diag_in[kk].astype(f32)).astype(bf16)
        cut = pl.ds(b0, half)
        returns.append(
            send(psum.at[dge, cut], ret_in.at[dge, cut], (re_s, re_r), 2 * dge + 1, dge)
        )

    hidden(0)
    down(0)
    for dge in range(1, n_ep):
        if dge > 1:
            for wc in [wcopies[dge]]:
                wc.wait_recv()
        else:
            wcopies[1].wait_recv()
            for dk in range(n_z):
                age[3, dk].wait_recv()
            to_sibling(3)
        sib[dge].wait_recv()
        hidden(dge)
        if dge > 1:
            finish(dge - 1)
        down(dge)
    finish(3)
    pair[0].wait_recv()
    finish_late(1)
    finish_late(2)

    for rc in returns:
        rc.wait_recv()

    def combine(kk):
        return chip_sum(0, kk) + ret_in[1, kk].astype(f32) + ret_in[2, kk].astype(f32)

    zcopies2 = []
    for d in range(1, n_z):
        kk = xor(k, d, n_z)
        zout[d] = combine(kk).astype(bf16)
        zc = remote(zout.at[d], zin.at[d], rz_s.at[d], rz_r.at[d], e, 2 * kk + c)
        zc.start()
        zcopies2.append(zc)
    total = combine(k) + ALPHA * xall[e, c, k].astype(f32)
    for d in range(1, n_z):
        zcopies2[d - 1].wait_recv()
        total = total + zin[d].astype(f32)
    final = norm_rows(total, 1.0)
    cols = width // n_tp
    for j in range(n_tp):
        oout[j] = final[:, j * cols : (j + 1) * cols]
    ocopies = []
    for d in range(1, n_tp):
        peer = xor(t, d, n_tp)
        oc = remote(oout.at[peer], oin.at[t], o_s.at[d], o_r.at[d], e, peer)
        oc.start()
        ocopies.append(oc)
    oin[t] = oout[t]
    for d in range(1, n_tp):
        peer = xor(t, d, n_tp)
        remote(oout.at[peer], oin.at[peer], o_s.at[d], o_r.at[d], e, peer).wait_recv()

    copy.wait_send()
    for group in (zcopies, agz, wcopies[1:], sends, zcopies2, ocopies):
        for each in group:
            each.wait_send()
    for group in (age, sib, pair):
        for each in group.values():
            each.wait_send()


def tail_kernel(rows_ref, state_ref, conv_ref, gain_ref, out_ref, nstate_ref, nconv_ref):
    rows, cols = out_ref.shape
    out_ref[...] = (rows_ref[...].reshape(rows, cols) * gain_ref[...]).astype(out_ref.dtype)
    nstate_ref[...] = state_ref[...]
    nconv_ref[...] = conv_ref[...]


def on_device(*args):
    tokens, routing, expert_gate = args[0], args[14], args[11]
    rows, width = tokens.shape
    n_ep, n_tp = lax.axis_size("ep"), lax.axis_size("tp")
    experts = expert_gate.shape[0] * n_ep
    capacity = max(2, 2 * rows * TOPK // experts)
    square = n_ep == 4 and n_tp >= 4 and n_tp & (n_tp - 1) == 0
    if capacity < rows or expert_gate.shape[0] != 1 or not square:
        return on_device_slots(*args)
    rr, n_z = rows // n_tp, n_tp // 2
    own, ff = args[3].shape[1], expert_gate.shape[2]
    bf16, f32 = jnp.bfloat16, jnp.float32
    operands = list(args)
    operands[0] = tokens.reshape(n_tp, rr, width)
    operands[1] = jnp.transpose(args[1], (1, 0, 2))
    for i in (14, 15):
        operands[i] = args[i].T
    for i in (8, 10, 20):
        operands[i] = args[i].reshape(1, -1)
    for i in (11, 12, 13):
        operands[i] = args[i][0]
    gain = operands.pop()
    in_hbm = (0, 3, 4, 9, 11, 12, 13, 16, 17, 18)
    vmem = pl.BlockSpec(memory_space=pltpu.VMEM)
    dma = pltpu.SemaphoreType.DMA
    wide_out, new_state, new_conv = pl.pallas_call(
        functools.partial(block_kernel, n_ep, n_tp),
        out_shape=(
            jax.ShapeDtypeStruct((n_tp, rr, width // n_tp), f32),
            jax.ShapeDtypeStruct((rows, own), f32),
            jax.ShapeDtypeStruct((3, rows, own), bf16),
        ),
        in_specs=[
            pl.BlockSpec(memory_space=pl.ANY) if i in in_hbm else vmem
            for i in range(len(operands))
        ],
        out_specs=(vmem, vmem, vmem),
        scratch_shapes=[
            pltpu.VMEM((n_tp, rr, width), bf16),
            pltpu.VMEM((width, own), bf16),
            pltpu.VMEM((width, own), bf16),
            pltpu.VMEM((own, width), bf16),
            pltpu.VMEM((width, ff), bf16),
            pltpu.VMEM((width, ff), bf16),
            pltpu.VMEM((ff, width), bf16),
            pltpu.VMEM(args[16].shape, bf16),
            pltpu.VMEM(args[17].shape, bf16),
            pltpu.VMEM(args[18].shape, bf16),
            pltpu.VMEM((2, n_z, rr, width), bf16),
            pltpu.VMEM((n_z, rr, width), bf16),
            pltpu.VMEM((n_z, rr, width), bf16),
            pltpu.VMEM((n_z, rr, width), bf16),
            pltpu.VMEM((n_ep, 2, n_z, rr, width), bf16),
            pltpu.VMEM((rows, ff), bf16),
            pltpu.VMEM((rows, args[16].shape[1]), bf16),
            pltpu.VMEM((n_ep, 2, n_z, rr, width), bf16),
            pltpu.VMEM((n_ep, n_z, rr, width), bf16),
            pltpu.VMEM((n_ep, n_z, rr, width), bf16),
            pltpu.VMEM((n_z, rr, width), bf16),
            pltpu.VMEM((n_ep, n_z, rr, width), bf16),
            pltpu.VMEM((n_z, rr, width), bf16),
            pltpu.VMEM((n_z, rr, width), bf16),
            pltpu.VMEM((n_tp, rr, width // n_tp), f32),
            pltpu.VMEM((n_ep, 8, rows), f32),
            pltpu.VMEM((n_ep, 8, rows), f32),
            dma((len(in_hbm),)),
            dma((2,)),
            dma((n_z,)),
            dma((n_z,)),
            dma((n_z,)),
            dma((n_z,)),
            dma((n_ep, n_z)),
            dma((n_ep, n_z)),
            dma((n_ep,)),
            dma((n_ep,)),
            dma((n_ep,)),
            dma((n_ep,)),
            dma((2 * n_ep,)),
            dma((2 * n_ep,)),
            dma((n_ep,)),
            dma((n_ep,)),
            dma((n_ep,)),
            dma((n_ep,)),
            dma((n_z,)),
            dma((n_z,)),
            dma((n_tp,)),
            dma((n_tp,)),
        ],
        compiler_params=pltpu.CompilerParams(
            collective_id=0, has_side_effects=True, vmem_limit_bytes=56 * 2**20
        ),
    )(*operands)
    layer_out, new_state, new_conv = pl.pallas_call(
        tail_kernel,
        out_shape=(
            jax.ShapeDtypeStruct((rows, own), bf16),
            jax.ShapeDtypeStruct((rows, own), f32),
            jax.ShapeDtypeStruct((3, rows, own), bf16),
        ),
        in_specs=[vmem] * 4,
        out_specs=(vmem,) * 3,
    )(wide_out, new_state, new_conv, gain)
    return layer_out, new_state, jnp.transpose(new_conv, (1, 0, 2))


def solution(mesh):
    return jax.shard_map(
        on_device,
        mesh=mesh,
        in_specs=(
            P("ep", None),
            P("ep", None, "tp"),
            P("ep", "tp"),
            P(None, "tp"),
            P(None, "tp"),
            P(None, "tp"),
            P("tp", None, None),
            P("tp", None, None),
            P("tp"),
            P("tp", None),
            P(),
            P("ep", None, "tp"),
            P("ep", None, "tp"),
            P("ep", "tp", None),
            P("ep", None),
            P("ep", None),
            P(None, "tp"),
            P(None, "tp"),
            P("tp", None),
            P(),
            P("tp"),
        ),
        out_specs=(P("ep", "tp"), P("ep", "tp"), P("ep", None, "tp")),
        check_vma=False,
    )
```

```python
import functools

import jax
import jax.numpy as jnp
from jax import lax
from jax.experimental import pallas as pl
from jax.experimental.pallas import tpu as pltpu
from jax.sharding import PartitionSpec as P

D = 2048
TOPK = 2


ALPHA = 8.0**0.25
RATE_SCALE = 8.0
NORM_EPS = 1e-05


def norm_rows(values, gain_vec):
    centre = values - jnp.mean(values, axis=-1, keepdims=True)
    spread = jnp.mean(centre * centre, axis=-1, keepdims=True)
    return centre * lax.rsqrt(spread + NORM_EPS) * gain_vec


def on_device_slots(
    tokens,
    conv_state,
    rec_state,
    gate_proj,
    input_proj,
    conv_taps,
    decay_blocks,
    input_blocks,
    decay_param,
    out_proj,
    first_gain,
    expert_gate,
    expert_up,
    expert_down,
    routing,
    route_weight,
    dense_gate,
    dense_up,
    dense_down,
    mix_weight,
    second_gain,
):
    count_rows = tokens.shape[0]
    gated = jnp.dot(tokens, gate_proj, preferred_element_type=jnp.float32).astype(jnp.bfloat16)
    inputs = jnp.dot(tokens, input_proj, preferred_element_type=jnp.float32).astype(jnp.bfloat16)
    window = jnp.concatenate([conv_state, inputs[:, None, :]], axis=1)
    convolved = jnp.sum(
        window.astype(jnp.float32) * conv_taps.astype(jnp.float32)[None], axis=1
    ).astype(jnp.bfloat16)
    local_heads = decay_blocks.shape[0]
    heads_view = convolved.reshape(count_rows, local_heads, -1)
    recur_gate = jax.nn.sigmoid(
        jnp.einsum("bhi,hij->bhj", heads_view, decay_blocks, preferred_element_type=jnp.float32)
    ).reshape(count_rows, -1)
    input_gate = jax.nn.sigmoid(
        jnp.einsum("bhi,hij->bhj", heads_view, input_blocks, preferred_element_type=jnp.float32)
    ).reshape(count_rows, -1)
    log_decay = -RATE_SCALE * recur_gate * jax.nn.softplus(-decay_param)
    new_state = jnp.exp(log_decay) * rec_state + jnp.sqrt(
        -jnp.expm1(2.0 * log_decay)
    ) * input_gate * convolved.astype(jnp.float32)
    mixed_rows = (new_state * jax.nn.gelu(gated.astype(jnp.float32), approximate=True)).astype(
        jnp.bfloat16
    )
    partial_mix = jnp.dot(mixed_rows, out_proj, preferred_element_type=jnp.float32)
    mixed = lax.psum(partial_mix.astype(jnp.bfloat16), "tp").astype(jnp.float32)
    normed = norm_rows(ALPHA * tokens.astype(jnp.float32) + mixed, first_gain).astype(jnp.bfloat16)
    tp_index = lax.axis_index("tp")
    tp_count = lax.axis_size("tp")
    own_width = D // tp_count
    own_normed = lax.dynamic_slice_in_dim(normed, tp_index * own_width, own_width, 1)
    local_experts = expert_gate.shape[0]
    ep_count = lax.axis_size("ep")
    experts = local_experts * ep_count
    capacity = max(2, 2 * count_rows * TOPK // experts)
    flat_routes = routing.reshape(-1)
    labels = jnp.arange(experts, dtype=jnp.int32)
    onehot = (flat_routes[:, None] == labels[None, :]).astype(jnp.int32)
    earlier = jnp.cumsum(onehot, axis=0) - onehot
    slot_index = jnp.sum(earlier * onehot, axis=1)
    target = flat_routes * capacity + slot_index
    placed = (target[:, None] == jnp.arange(experts * capacity, dtype=jnp.int32)[None, :]).astype(
        jnp.bfloat16
    )
    token_slots = jnp.sum(placed.reshape(count_rows, TOPK, experts * capacity), axis=1)
    dispatch = jnp.dot(token_slots.T, normed, preferred_element_type=jnp.float32).astype(
        jnp.bfloat16
    )
    arrived = lax.all_to_all(
        dispatch.reshape(experts, capacity, D), "ep", split_axis=0, concat_axis=1, tiled=True
    )
    gate_val = jnp.einsum("erd,edf->erf", arrived, expert_gate, preferred_element_type=jnp.float32)
    up_val = jnp.einsum("erd,edf->erf", arrived, expert_up, preferred_element_type=jnp.float32)
    hidden = (jax.nn.silu(gate_val) * up_val).astype(jnp.bfloat16)
    partial_out = jnp.einsum(
        "erf,efd->erd", hidden, expert_down, preferred_element_type=jnp.float32
    )
    reduced = lax.psum_scatter(
        partial_out.astype(jnp.bfloat16), "tp", scatter_dimension=2, tiled=True
    )
    returned = lax.all_to_all(reduced, "ep", split_axis=1, concat_axis=0, tiled=True)
    returned = returned.reshape(experts * capacity, own_width)
    picked = jnp.dot(placed, returned, preferred_element_type=jnp.float32).reshape(
        count_rows, TOPK, own_width
    )
    routed_sum = jnp.sum(route_weight[:, :, None] * picked, axis=1)
    dense_g = jnp.dot(normed, dense_gate, preferred_element_type=jnp.float32)
    dense_u = jnp.dot(normed, dense_up, preferred_element_type=jnp.float32)
    dense_hidden = (jax.nn.silu(dense_g) * dense_u).astype(jnp.bfloat16)
    dense_part = jnp.dot(dense_hidden, dense_down, preferred_element_type=jnp.float32)
    dense_out = lax.psum_scatter(
        dense_part.astype(jnp.bfloat16), "tp", scatter_dimension=1, tiled=True
    ).astype(jnp.float32)
    mix = jax.nn.sigmoid(jnp.dot(normed, mix_weight, preferred_element_type=jnp.float32))
    combined = ALPHA * own_normed.astype(jnp.float32) + routed_sum + mix[:, None] * dense_out
    row_total, row_square = lax.psum(
        (jnp.sum(combined, axis=1), jnp.sum(combined * combined, axis=1)), "tp"
    )
    row_mean = row_total / D
    row_var = row_square / D - row_mean * row_mean
    layer_out = (
        (combined - row_mean[:, None]) * lax.rsqrt(row_var[:, None] + NORM_EPS) * second_gain
    ).astype(jnp.bfloat16)
    return (layer_out, new_state, window[:, 1:])


MESH = pl.DeviceIdType.MESH


def xor(left, right, count):
    total, bit = 0, 1
    while bit < count:
        lbit, rbit = (left // bit) % 2, (right // bit) % 2
        total = total + bit * (lbit + rbit - 2 * lbit * rbit)
        bit *= 2
    return total


def block_kernel(
    n_ep,
    n_tp,
    tokens_hbm,
    conv_ref,
    state_ref,
    gproj_hbm,
    iproj_hbm,
    taps_ref,
    dblk_ref,
    iblk_ref,
    dparam_ref,
    oproj_hbm,
    fgain_ref,
    eg_hbm,
    eu_hbm,
    ed_hbm,
    routing_ref,
    rweight_ref,
    dg_hbm,
    du_hbm,
    dd_hbm,
    mixw_ref,
    oin,
    nstate_ref,
    nconv_ref,
    tok,
    gproj,
    iproj,
    oproj,
    eg,
    eu,
    ed,
    dg,
    du,
    dd,
    pmix,
    pmix_in,
    smix,
    smix_in,
    xall,
    hid,
    dhid,
    part,
    part_in,
    psum,
    diag_in,
    ret_in,
    zout,
    zin,
    oout,
    wsend,
    wrecv,
    wsem,
    bpair,
    bz_s,
    bz_r,
    agz_s,
    agz_r,
    age_s,
    age_r,
    sib_s,
    sib_r,
    rp_s,
    rp_r,
    re_s,
    re_r,
    rd_s,
    rd_r,
    w_s,
    w_r,
    rz_s,
    rz_r,
    o_s,
    o_r,
):
    f32, bf16 = jnp.float32, jnp.bfloat16
    e, t = lax.axis_index("ep"), lax.axis_index("tp")
    n_z = n_tp // 2
    c, k = t % 2, t // 2
    other = 1 - c
    sibling = 2 * k + other
    rr, width = tok.shape[1], tok.shape[2]
    rows = n_tp * rr
    wide = min(512, width)

    loads = [
        pltpu.make_async_copy(a, b, wsem.at[i])
        for i, (a, b) in enumerate(
            [
                (tokens_hbm, tok),
                (iproj_hbm, iproj),
                (gproj_hbm, gproj),
                (oproj_hbm, oproj),
                (dg_hbm, dg),
                (du_hbm, du),
                (dd_hbm, dd),
                (eg_hbm, eg),
                (eu_hbm, eu),
                (ed_hbm, ed),
            ]
        )
    ]
    for load in loads[:4]:
        load.start()

    barrier = pltpu.get_barrier_semaphore()
    for d in range(1, n_tp):
        pl.semaphore_signal(barrier, inc=1, device_id=(e, xor(t, d, n_tp)), device_id_type=MESH)
    for d in range(1, n_ep):
        pl.semaphore_signal(barrier, inc=1, device_id=(xor(e, d, n_ep), t), device_id_type=MESH)

    def remote(src, dst, send, recv, ep, tp):
        return pltpu.make_async_remote_copy(
            src_ref=src, dst_ref=dst, send_sem=send, recv_sem=recv,
            device_id=(ep, tp), device_id_type=MESH,
        )

    route, rweight = routing_ref[...], rweight_ref[...]
    for d in range(n_ep):
        row = jnp.zeros((1, rows), f32)
        for j in range(TOPK):
            row = row + jnp.where(
                route[j : j + 1] == xor(e, d, n_ep), rweight[j : j + 1], 0.0
            )
        wsend[d] = jnp.broadcast_to(row, (8, rows))

    loads[0].wait()
    loads[1].wait()
    tokens = tok[...].reshape(rows, width)
    inputs = jnp.dot(tokens, iproj[...], preferred_element_type=f32).astype(bf16)
    taps = taps_ref[...].astype(f32)
    conv = inputs.astype(f32) * taps[3:4]
    for j in range(3):
        conv = conv + conv_ref[j].astype(f32) * taps[j : j + 1]
    nconv_ref[0] = conv_ref[1]
    nconv_ref[1] = conv_ref[2]
    nconv_ref[2] = inputs
    conv = conv.astype(bf16)
    heads, blk = dblk_ref.shape[0], dblk_ref.shape[1]

    def by_head(ref):
        parts = [
            jnp.dot(conv[:, h * blk : (h + 1) * blk], ref[h], preferred_element_type=f32)
            for h in range(heads)
        ]
        return jax.nn.sigmoid(jnp.concatenate(parts, axis=1))

    recur_gate, input_gate = by_head(dblk_ref), by_head(iblk_ref)
    neg = -dparam_ref[...]
    soft = jnp.maximum(neg, 0.0) + jnp.log1p(jnp.exp(-jnp.abs(neg)))
    log_decay = -RATE_SCALE * recur_gate * soft
    decay = jnp.exp(log_decay)
    new_state = decay * state_ref[...] + jnp.sqrt(
        -jnp.tanh(log_decay) * (decay * decay + 1.0)
    ) * input_gate * conv.astype(f32)
    nstate_ref[...] = new_state
    loads[2].wait()
    loads[3].wait()
    for load in loads[4:]:
        load.start()
    gated = jnp.dot(tokens, gproj[...], preferred_element_type=f32).astype(bf16).astype(f32)
    mixed = (new_state * jax.nn.gelu(gated, approximate=True)).astype(bf16)
    for n0 in range(0, width, wide):
        val = jnp.dot(mixed, oproj[:, n0 : n0 + wide], preferred_element_type=f32).astype(bf16)
        for j in range(n_tp):
            pmix[j % 2, j // 2, :, n0 : n0 + wide] = val[j * rr : (j + 1) * rr]
    pl.semaphore_wait(barrier, n_tp - 1 + n_ep - 1)

    copy = remote(pmix.at[other], pmix_in, bpair.at[0], bpair.at[1], e, sibling)
    copy.start()
    wcopies = [None]
    for d in range(1, n_ep):
        wc = remote(wsend.at[d], wrecv.at[d], w_s.at[d], w_r.at[d], xor(e, d, n_ep), t)
        wc.start()
        wcopies.append(wc)
    copy.wait_recv()
    zcopies = []
    for d in range(1, n_z):
        kk = xor(k, d, n_z)
        smix[d] = (pmix[c, kk].astype(f32) + pmix_in[kk].astype(f32)).astype(bf16)
        zc = remote(smix.at[d], smix_in.at[d], bz_s.at[d], bz_r.at[d], e, 2 * kk + c)
        zc.start()
        zcopies.append(zc)
    mix_rows = pmix[c, k].astype(f32) + pmix_in[k].astype(f32)
    mix_rows = mix_rows + ALPHA * tok[t].astype(f32)
    for d in range(1, n_z):
        zcopies[d - 1].wait_recv()
        mix_rows = mix_rows + smix_in[d].astype(f32)
    normed = norm_rows(mix_rows, fgain_ref[...]).astype(bf16)
    xall[e, c, k] = normed

    agz, age, sib, pair = [], {}, {}, {}
    half = n_z // 2

    def slot(dge, dk):
        return xall.at[xor(e, dge, n_ep), c, xor(k, dk, n_z)]

    for d in range(1, n_z):
        zc = remote(
            slot(0, 0), slot(0, 0), agz_s.at[d], agz_r.at[d], e, 2 * xor(k, d, n_z) + c
        )
        zc.start()
        agz.append(zc)

    def to_ep(dge, dk, origin=0):
        src = slot(origin, dk)
        at = dge ^ origin
        ec = remote(src, src, age_s.at[at, dk], age_r.at[at, dk], xor(e, dge, n_ep), t)
        ec.start()
        age[at, dk] = ec

    def to_sibling(dge):
        src = xall.at[xor(e, dge, n_ep), c]
        sib[dge] = remote(src, src, sib_s.at[dge], sib_r.at[dge], e, sibling)
        sib[dge].start()

    def forward(dk):
        age[1, dk].wait_recv()
        age[2, dk].wait_recv()
        if dk < half:
            to_ep(2, dk, 1)
        else:
            to_ep(1, dk, 2)

    for dk in range(n_z):
        if dk:
            agz[dk - 1].wait_recv()
        to_ep(1, dk)
        to_ep(2, dk)
    to_sibling(0)

    ff = eg.shape[1]
    forward(0)
    sib[0].wait_recv()
    for i in (4, 5):
        loads[i].wait()
    rows_own = xall[e].reshape(rows, width)
    dhid[...] = (
        jax.nn.silu(jnp.dot(rows_own, dg[...], preferred_element_type=f32))
        * jnp.dot(rows_own, du[...], preferred_element_type=f32)
    ).astype(bf16)
    for dk in range(1, n_z):
        forward(dk)
    to_sibling(1)
    to_sibling(2)
    mix = jax.nn.sigmoid(
        jnp.sum(
            rows_own.astype(f32) * mixw_ref[...].astype(f32).reshape(1, width),
            axis=1,
            keepdims=True,
        )
    )
    for i in (6, 7, 8, 9):
        loads[i].wait()

    def hidden(dge):
        x = xall[xor(e, dge, n_ep)].reshape(rows, width)
        for f0 in range(0, ff, 256):
            f1 = min(ff, f0 + 256)
            gate_val = jnp.dot(x, eg[:, f0:f1], preferred_element_type=f32)
            up_val = jnp.dot(x, eu[:, f0:f1], preferred_element_type=f32)
            hid[:, f0:f1] = (jax.nn.silu(gate_val) * up_val).astype(bf16)

    def down(dge):
        row = (wrecv if dge else wsend)[dge][:1]
        across = lax.broadcasted_iota(jnp.int32, (rows, rows), 0)
        along = lax.broadcasted_iota(jnp.int32, (rows, rows), 1)
        col = jnp.sum(jnp.where(across == along, row, 0.0), axis=1, keepdims=True)
        weights = jnp.concatenate(
            [col[j * rr : (j + 1) * rr] for cc in range(2) for j in range(cc, n_tp, 2)], axis=0
        )
        for n0 in range(0, width, wide):
            cut = slice(n0, n0 + wide)
            val = weights * jnp.dot(hid[...], ed[:, cut], preferred_element_type=f32)
            if dge == 0:
                val = val + mix * jnp.dot(dhid[...], dd[:, cut], preferred_element_type=f32)
            part[dge, :, :, :, cut] = val.astype(bf16).reshape(2, n_z, rr, wide)
        pair[dge] = remote(
            part.at[dge, other], part_in.at[dge], rp_s.at[dge], rp_r.at[dge], e, sibling
        )
        pair[dge].start()

    def chip_sum(dge, kk):
        return part[dge, c, kk].astype(f32) + part_in[dge, kk].astype(f32)

    order = list(range(1, n_z)) + [0]
    by_first, by_second = order[0::2], order[1::2]
    early = {1: by_first, 2: by_second}
    sends = []

    def send(src, dst, send_sem, recv_sem, dge):
        rc = remote(src, dst, send_sem, recv_sem, xor(e, dge, n_ep), t)
        rc.start()
        sends.append(rc)
        return rc

    returns, diagonal = {}, {}

    def to_owner(dge, dk):
        returns[dge, dk] = send(
            psum.at[dge, dk], ret_in.at[dge, dk], re_s.at[dge, dk], re_r.at[dge, dk], dge
        )

    def finish(dge):
        pair[dge].wait_recv()
        for dk in order if dge == 3 else early[dge]:
            psum[dge, dk] = chip_sum(dge, xor(k, dk, n_z)).astype(bf16)
            if dge == 3:
                diagonal[dk] = send(
                    psum.at[3, dk],
                    diag_in.at[dk],
                    rd_s.at[dk],
                    rd_r.at[dk],
                    1 if dk in by_first else 2,
                )
            else:
                to_owner(dge, dk)

    for dge in range(1, n_ep):
        wcopies[dge].wait_recv()
        sib[dge].wait_recv()
        hidden(dge)
        if dge == 2:
            for dk in range(n_z):
                age[3, dk].wait_recv()
            to_sibling(3)
        if dge > 1:
            finish(dge - 1)
        down(dge)
    finish(3)
    hidden(0)
    down(0)
    for dk in order:
        dge = 2 if dk in by_first else 1
        diagonal[dk].wait_recv()
        psum[dge, dk] = (
            chip_sum(dge, xor(k, dk, n_z)) + diag_in[dk].astype(f32)
        ).astype(bf16)
        to_owner(dge, dk)
    pair[0].wait_recv()

    def combine(dk):
        returns[1, dk].wait_recv()
        returns[2, dk].wait_recv()
        return (
            chip_sum(0, xor(k, dk, n_z)) + ret_in[1, dk].astype(f32) + ret_in[2, dk].astype(f32)
        )

    zcopies2 = []
    for d in range(1, n_z):
        kk = xor(k, d, n_z)
        zout[d] = combine(d).astype(bf16)
        zc = remote(zout.at[d], zin.at[d], rz_s.at[d], rz_r.at[d], e, 2 * kk + c)
        zc.start()
        zcopies2.append(zc)
    total = combine(0) + ALPHA * xall[e, c, k].astype(f32)
    for d in range(1, n_z):
        zcopies2[d - 1].wait_recv()
        total = total + zin[d].astype(f32)
    final = norm_rows(total, 1.0)
    cols = width // n_tp
    for j in range(n_tp):
        oout[j] = final[:, j * cols : (j + 1) * cols]
    ocopies = []
    for d in range(1, n_tp):
        peer = xor(t, d, n_tp)
        oc = remote(oout.at[peer], oin.at[t], o_s.at[d], o_r.at[d], e, peer)
        oc.start()
        ocopies.append(oc)
    oin[t] = oout[t]
    for d in range(1, n_tp):
        peer = xor(t, d, n_tp)
        remote(oout.at[peer], oin.at[peer], o_s.at[d], o_r.at[d], e, peer).wait_recv()

    copy.wait_send()
    for group in (zcopies, agz, wcopies[1:], sends, zcopies2, ocopies):
        for each in group:
            each.wait_send()
    for group in (age, sib, pair):
        for each in group.values():
            each.wait_send()


def tail_kernel(rows_ref, state_ref, conv_ref, gain_ref, out_ref, nstate_ref, nconv_ref):
    rows, cols = out_ref.shape
    out_ref[...] = (rows_ref[...].reshape(rows, cols) * gain_ref[...]).astype(out_ref.dtype)
    nstate_ref[...] = state_ref[...]
    nconv_ref[...] = conv_ref[...]


def on_device(*args):
    tokens, routing, expert_gate = args[0], args[14], args[11]
    rows, width = tokens.shape
    n_ep, n_tp = lax.axis_size("ep"), lax.axis_size("tp")
    experts = expert_gate.shape[0] * n_ep
    capacity = max(2, 2 * rows * TOPK // experts)
    square = n_ep == 4 and n_tp >= 4 and n_tp & (n_tp - 1) == 0
    if capacity < rows or expert_gate.shape[0] != 1 or not square:
        return on_device_slots(*args)
    rr, n_z = rows // n_tp, n_tp // 2
    own, ff = args[3].shape[1], expert_gate.shape[2]
    bf16, f32 = jnp.bfloat16, jnp.float32
    operands = list(args)
    operands[0] = tokens.reshape(n_tp, rr, width)
    operands[1] = jnp.transpose(args[1], (1, 0, 2))
    for i in (14, 15):
        operands[i] = args[i].T
    for i in (8, 10, 20):
        operands[i] = args[i].reshape(1, -1)
    for i in (11, 12, 13):
        operands[i] = args[i][0]
    gain = operands.pop()
    in_hbm = (0, 3, 4, 9, 11, 12, 13, 16, 17, 18)
    vmem = pl.BlockSpec(memory_space=pltpu.VMEM)
    dma = pltpu.SemaphoreType.DMA
    wide_out, new_state, new_conv = pl.pallas_call(
        functools.partial(block_kernel, n_ep, n_tp),
        out_shape=(
            jax.ShapeDtypeStruct((n_tp, rr, width // n_tp), f32),
            jax.ShapeDtypeStruct((rows, own), f32),
            jax.ShapeDtypeStruct((3, rows, own), bf16),
        ),
        in_specs=[
            pl.BlockSpec(memory_space=pl.ANY) if i in in_hbm else vmem
            for i in range(len(operands))
        ],
        out_specs=(vmem, vmem, vmem),
        scratch_shapes=[
            pltpu.VMEM((n_tp, rr, width), bf16),
            pltpu.VMEM((width, own), bf16),
            pltpu.VMEM((width, own), bf16),
            pltpu.VMEM((own, width), bf16),
            pltpu.VMEM((width, ff), bf16),
            pltpu.VMEM((width, ff), bf16),
            pltpu.VMEM((ff, width), bf16),
            pltpu.VMEM(args[16].shape, bf16),
            pltpu.VMEM(args[17].shape, bf16),
            pltpu.VMEM(args[18].shape, bf16),
            pltpu.VMEM((2, n_z, rr, width), bf16),
            pltpu.VMEM((n_z, rr, width), bf16),
            pltpu.VMEM((n_z, rr, width), bf16),
            pltpu.VMEM((n_z, rr, width), bf16),
            pltpu.VMEM((n_ep, 2, n_z, rr, width), bf16),
            pltpu.VMEM((rows, ff), bf16),
            pltpu.VMEM((rows, args[16].shape[1]), bf16),
            pltpu.VMEM((n_ep, 2, n_z, rr, width), bf16),
            pltpu.VMEM((n_ep, n_z, rr, width), bf16),
            pltpu.VMEM((n_ep, n_z, rr, width), bf16),
            pltpu.VMEM((n_z, rr, width), bf16),
            pltpu.VMEM((n_ep, n_z, rr, width), bf16),
            pltpu.VMEM((n_z, rr, width), bf16),
            pltpu.VMEM((n_z, rr, width), bf16),
            pltpu.VMEM((n_tp, rr, width // n_tp), f32),
            pltpu.VMEM((n_ep, 8, rows), f32),
            pltpu.VMEM((n_ep, 8, rows), f32),
            dma((len(in_hbm),)),
            dma((2,)),
            dma((n_z,)),
            dma((n_z,)),
            dma((n_z,)),
            dma((n_z,)),
            dma((n_ep, n_z)),
            dma((n_ep, n_z)),
            dma((n_ep,)),
            dma((n_ep,)),
            dma((n_ep,)),
            dma((n_ep,)),
            dma((n_ep, n_z)),
            dma((n_ep, n_z)),
            dma((n_z,)),
            dma((n_z,)),
            dma((n_ep,)),
            dma((n_ep,)),
            dma((n_z,)),
            dma((n_z,)),
            dma((n_tp,)),
            dma((n_tp,)),
        ],
        compiler_params=pltpu.CompilerParams(
            collective_id=0, has_side_effects=True, vmem_limit_bytes=56 * 2**20
        ),
    )(*operands)
    layer_out, new_state, new_conv = pl.pallas_call(
        tail_kernel,
        out_shape=(
            jax.ShapeDtypeStruct((rows, own), bf16),
            jax.ShapeDtypeStruct((rows, own), f32),
            jax.ShapeDtypeStruct((3, rows, own), bf16),
        ),
        in_specs=[vmem] * 4,
        out_specs=(vmem,) * 3,
    )(wide_out, new_state, new_conv, gain)
    return layer_out, new_state, jnp.transpose(new_conv, (1, 0, 2))


def solution(mesh):
    return jax.shard_map(
        on_device,
        mesh=mesh,
        in_specs=(
            P("ep", None),
            P("ep", None, "tp"),
            P("ep", "tp"),
            P(None, "tp"),
            P(None, "tp"),
            P(None, "tp"),
            P("tp", None, None),
            P("tp", None, None),
            P("tp"),
            P("tp", None),
            P(),
            P("ep", None, "tp"),
            P("ep", None, "tp"),
            P("ep", "tp", None),
            P("ep", None),
            P("ep", None),
            P(None, "tp"),
            P(None, "tp"),
            P("tp", None),
            P(),
            P("tp"),
        ),
        out_specs=(P("ep", "tp"), P("ep", "tp"), P("ep", None, "tp")),
        check_vma=False,
    )
```
